32 devices in a mesh: sp: 8 (over z, x), dp: 4 (over y, core).
Axes of the slice: x: 2, y: 2, z: 4, core: 2. Of those that a mesh axis runs over, the one named last changes fastest.
Arguments:
- residual_in: bfloat16 [4, 1024, 2048], P('dp', 'sp'), may hold values from -6 to 6
- query_rows: bfloat16 [4, 1024, 1024], P('dp', 'sp'), may hold values from -40 to 40
- key_rows: bfloat16 [4, 1024, 1024], P('dp', 'sp'), may hold values from -40 to 40
- value_rows: bfloat16 [4, 1024, 1024], P('dp', 'sp'), may hold values from -6 to 6
- gate_sums: float32 [4, 16, 1024], P('dp', 'sp'), as said below
- out_weight: bfloat16 [1024, 2048], replicated, may hold values from -0.1875 to 0.1875
- mix_gain: float32 [2048], replicated, may hold values from 0.1 to 1.9
- ffn_gain: float32 [2048], replicated, may hold values from 0.1 to 1.9
- expert_ids: int32 [4, 1024, 4], P('dp', 'sp'), may hold values from 0 to 31, all different within a row; in each aligned block of 128 rows (0 to 127, 128 to 255, ..., all dimensions but the last counted through in order) at most 32 rows name the same one
- route_weights: float32 [4, 1024, 4], P('dp', 'sp'), may hold values from 0.3 to 2
- expert_gate: bfloat16 [32, 2048, 512], P(('sp', 'dp')), may hold values from -0.125 to 0.125
- expert_up: bfloat16 [32, 2048, 512], P(('sp', 'dp')), may hold values from -0.125 to 0.125
- expert_down: bfloat16 [32, 512, 2048], P(('sp', 'dp')), may hold values from -0.25 to 0.25
- shared_gate: bfloat16 [2048, 512], replicated, may hold values from -0.125 to 0.125
- shared_up: bfloat16 [2048, 512], replicated, may hold values from -0.125 to 0.125
- shared_down: bfloat16 [512, 2048], replicated, may hold values from -0.25 to 0.25
Outputs:
- result_rows: bfloat16 [4, 1024, 2048], P('dp', 'sp')
The draws below stay inside these ranges and needn't reach their ends.
Inputs may be any that keep to these rules, and one draw needn't show every extreme that they name: `expert_ids`: each row names 4 different experts. In the rows of one device no expert is named more than 32 times, a bound that some block reaches in some devices' rows. `gate_sums`: Non-increasing along positions for every sequence and head.
All inputs are finite; a program needn't handle non-finite values.
Results may differ from the reference program's by a relative error of at most 0.0071.
Values may be sent and summed in bfloat16 or wider, within the bound.
A program may use at most 128 MiB of HBM per device.

```python
import math
import jax
import jax.numpy as jnp
import numpy as np
from jax import lax

D = 2048
HEADS = 16
HEAD_DIM = 64
EFF = 512
TOPK = 4
TOK_DEV = 128
ATT = 1024
SEQUENCE_COUNT = 4
SEQUENCE_LENGTH = 1024
EXPERTS = 32
CAP = 32


def drawn(key):
    base = jax.random.fold_in(key, 17)
    first, second = jax.random.split(base, 2)
    query_draw = jnp.clip(jax.random.normal(first, (SEQUENCE_COUNT, SEQUENCE_LENGTH, ATT), jnp.float32), -6.0, 6.0)
    key_draw = jnp.clip(jax.random.normal(second, (SEQUENCE_COUNT, SEQUENCE_LENGTH, ATT), jnp.float32), -6.0, 6.0)
    return (query_draw, key_draw)


def draw_query_rows(key, part):
    return drawn(key)[0].astype(jnp.bfloat16)


def draw_key_rows(key, part):
    return drawn(key)[1].astype(jnp.bfloat16)


def draw_gate_sums(key, part):
    base = jax.random.fold_in(key, 29)
    first, second, third, fourth, fifth, sixth_draw, seventh_draw = jax.random.split(base, 7)
    order = jax.random.permutation(first, HEADS)
    fast = order < HEADS // 2
    fast_rate = jnp.exp(jax.random.uniform(second, (SEQUENCE_COUNT, HEADS), jnp.float32, jnp.log(1.0 / 60.0), jnp.log(1.0 / 25.0)))
    slow_total = jnp.exp(jax.random.uniform(third, (SEQUENCE_COUNT, HEADS), jnp.float32, jnp.log(0.2), jnp.log(0.8)))
    rate = jnp.where(fast[None, :], fast_rate, slow_total / SEQUENCE_LENGTH)
    rough = jnp.exp(jax.random.uniform(fourth, (SEQUENCE_COUNT, HEADS, SEQUENCE_LENGTH), jnp.float32, jnp.log(0.5), jnp.log(2.0)))
    block_factor = jnp.exp(jax.random.uniform(fifth, (SEQUENCE_COUNT, SEQUENCE_LENGTH // TOK_DEV), jnp.float32, 0.0, jnp.log(3.0)))
    block_factor = jnp.repeat(block_factor, TOK_DEV, axis=1)
    step_values = -rate[:, :, None] * rough * block_factor[:, None, :]
    spike_position = jax.random.randint(sixth_draw, (SEQUENCE_COUNT, 3), 0, SEQUENCE_LENGTH)
    spike_length = jnp.log(jax.random.uniform(seventh_draw, (SEQUENCE_COUNT, 3), jnp.float32, 0.5, 0.8))
    token_positions = jnp.arange(SEQUENCE_LENGTH)
    match_count = jnp.sum(jnp.where(token_positions[None, None, :] == spike_position[:, :, None], spike_length[:, :, None], 0.0), axis=1)
    slow_mask = jnp.where(fast, 0.0, 1.0)
    step_values = step_values + slow_mask[None, :, None] * match_count[:, None, :]
    return jnp.cumsum(step_values, axis=2)


def block_scale(rng, shape, cuts, smallest, largest):
    def one(position, parts):
        heights = jax.random.uniform(jax.random.fold_in(jax.random.fold_in(rng, 6), position), (parts,), jnp.float32, smallest / len(cuts), largest / len(cuts))
        return jnp.repeat(jnp.exp(heights), shape[position] // parts).reshape((-1,) + (1,) * (len(shape) - position - 1))

    level = one(*cuts[0])
    for cut in cuts[1:]:
        level = level * one(*cut)
    return level


def assign_block(rng, own, number, rows, number_of, top, reach, lean):
    ranking = jax.random.permutation(rng, number_of)
    packed, usual = load_shares(number_of, rows * top, reach, lean, True), load_shares(number_of, rows * top, reach, lean, False)
    places = jnp.arange(number_of)

    def named(tallies, rotation):
        used = int((tallies > 0).sum())
        fixed = max(1, used // 4)
        passed = fixed + (places - fixed + rotation * (used - fixed)) % max(1, number_of - fixed)
        return jnp.zeros((number_of,), jnp.int32).at[ranking[jnp.where(places < fixed, places, passed)]].set(jnp.asarray(tallies, jnp.int32))

    tallies = jnp.where(number % 4 == 0, named(packed, number // 4), named(usual, number - number // 4 - 1))
    mixed = jax.random.permutation(jax.random.fold_in(own, 3), number_of)
    source_of, receiver = mixed[0:number_of // 2 * 2:2], mixed[1:number_of // 2 * 2:2]
    slack = jnp.minimum(tallies[source_of] - 1, reach - tallies[receiver]) // 2
    slack = jnp.where((source_of == ranking[0]) | (receiver == ranking[0]) | (tallies[receiver] == 0), 0, jnp.maximum(slack, 0))
    passed = jax.random.randint(jax.random.fold_in(own, 4), (number_of // 2,), 0, 1 << 20) % (slack + 1)
    tallies = tallies.at[source_of].add(-passed).at[receiver].add(passed)
    labels = jnp.searchsorted(jnp.cumsum(tallies), jnp.arange(rows * top), side="right").astype(jnp.int32)
    listing = labels.reshape(top, rows).T
    listing = listing[jax.random.permutation(jax.random.fold_in(own, 1), rows)]
    rotation = jax.random.randint(jax.random.fold_in(own, 2), (rows, 1), 0, top)
    return jnp.take_along_axis(listing, (jnp.arange(top)[None, :] + rotation) % top, axis=1)


def load_shares(count, total, limit, skew, full):
    portions = [(1 << 20) // math.isqrt(standing ** skew) + 1 for standing in range(1, count + 1)]
    largest = limit if full else min(limit, max(-(-total // count), total * portions[0] // sum(portions)))
    least = 1 if total - largest >= count - 1 else 0
    given, spare = [largest] + [least] * (count - 1), total - largest - least * (count - 1)
    while spare > 0:
        movable = [i for i in range(1, count) if given[i] < largest] or [i for i in range(1, count) if given[i] < limit]
        mass, remaining = sum([portions[i] for i in movable]), spare
        for i in movable:
            addition = min(limit - given[i], max(1, remaining * portions[i] // mass), spare)
            given[i] = given[i] + addition
            spare = spare - addition
    return np.array(given)


def centred(key, shape, deviation, most, pieces=(), kind=jnp.bfloat16):
    result = deviation * jax.random.normal(key, shape, jnp.float32)
    if pieces:
        result = result * block_scale(key, shape, pieces, -0.22, 0.18)
    return jnp.clip(result, -most, most).astype(kind)


def setup_inputs(seed: int = 0) -> dict:
    keys = jax.random.split(jax.random.key(seed), 17)
    residual_in = centred(keys[0], (SEQUENCE_COUNT, SEQUENCE_LENGTH, D), 1.0, 6.0, ((0, 4), (1, 8)))
    query_rows = draw_query_rows(jax.random.fold_in(keys[16], 71), 0)
    key_rows = draw_key_rows(jax.random.fold_in(keys[16], 71), 0)
    value_rows = centred(keys[3], (SEQUENCE_COUNT, SEQUENCE_LENGTH, ATT), 1.0, 6.0, ((0, 4), (1, 8)))
    gate_sums = draw_gate_sums(jax.random.fold_in(keys[16], 71), 0)
    out_weight = centred(keys[5], (ATT, D), ATT ** -0.5, 0.1875)
    mix_gain = jnp.clip(1.0 + 0.18 * jax.random.normal(keys[6], (D,), jnp.float32), 0.1, 1.9)
    ffn_gain = jnp.clip(1.0 + 0.18 * jax.random.normal(keys[7], (D,), jnp.float32), 0.1, 1.9)
    expert_ids_keys = jax.random.split(jax.random.fold_in(keys[8], 1), SEQUENCE_COUNT * SEQUENCE_LENGTH // TOK_DEV)
    expert_ids_turns = jax.random.permutation(jax.random.fold_in(keys[8], 3), SEQUENCE_COUNT * SEQUENCE_LENGTH // TOK_DEV)
    expert_ids = jax.vmap(lambda own, number: assign_block(jax.random.fold_in(keys[8], 2), own, number, TOK_DEV, EXPERTS, TOPK, CAP, 2))(expert_ids_keys, expert_ids_turns).reshape((SEQUENCE_COUNT, SEQUENCE_LENGTH, TOPK))
    route_weights = jnp.clip(jnp.exp(math.log(2.0) - 1.89712 * jax.random.uniform(keys[9], (SEQUENCE_COUNT, SEQUENCE_LENGTH, TOPK), jnp.float32) ** block_scale(keys[9], (SEQUENCE_COUNT, SEQUENCE_LENGTH, TOPK), ((0, 4), (1, 8)), -0.2, 0.2)), 0.3, 2.0)
    expert_gate = centred(keys[10], (EXPERTS, D, EFF), D ** -0.5, 0.125, ((0, 32),))
    expert_up = centred(keys[11], (EXPERTS, D, EFF), D ** -0.5, 0.125, ((0, 32),))
    expert_down = centred(keys[12], (EXPERTS, EFF, D), EFF ** -0.5, 0.25, ((0, 32),))
    shared_gate = centred(keys[13], (D, EFF), D ** -0.5, 0.125)
    shared_up = centred(keys[14], (D, EFF), D ** -0.5, 0.125)
    shared_down = centred(keys[15], (EFF, D), EFF ** -0.5, 0.25)
    return dict(residual_in=residual_in, query_rows=query_rows, key_rows=key_rows, value_rows=value_rows, gate_sums=gate_sums, out_weight=out_weight, mix_gain=mix_gain, ffn_gain=ffn_gain, expert_ids=expert_ids, route_weights=route_weights, expert_gate=expert_gate, expert_up=expert_up, expert_down=expert_down, shared_gate=shared_gate, shared_up=shared_up, shared_down=shared_down)


def reference(residual_in, query_rows, key_rows, value_rows, gate_sums, out_weight, mix_gain, ffn_gain, expert_ids, route_weights, expert_gate, expert_up, expert_down, shared_gate, shared_up, shared_down):
    score_scale = HEAD_DIM ** (-0.5)

    def one_head(pair_index):
        seq_index = pair_index // HEADS
        head_index = pair_index % HEADS
        zero = jnp.zeros((), jnp.int32)
        query_head = lax.dynamic_slice(query_rows, (seq_index, zero, head_index * HEAD_DIM), (1, SEQUENCE_LENGTH, HEAD_DIM))[0]
        key_head = lax.dynamic_slice(key_rows, (seq_index, zero, head_index * HEAD_DIM), (1, SEQUENCE_LENGTH, HEAD_DIM))[0]
        value_head = lax.dynamic_slice(value_rows, (seq_index, zero, head_index * HEAD_DIM), (1, SEQUENCE_LENGTH, HEAD_DIM))[0]
        sums_head = lax.dynamic_slice(gate_sums, (seq_index, head_index, zero), (1, 1, SEQUENCE_LENGTH))[0, 0]
        scores = jnp.dot(query_head, key_head.T, preferred_element_type=jnp.float32) * score_scale
        scores = scores + sums_head[:, None] - sums_head[None, :]
        causal_mask = jnp.arange(SEQUENCE_LENGTH)[None, :] <= jnp.arange(SEQUENCE_LENGTH)[:, None]
        scores = jnp.where(causal_mask, scores, -jnp.inf)
        peak = lax.optimization_barrier(jnp.max(scores, axis=1, keepdims=True))
        weights = jnp.exp(scores - peak)
        weights = (weights / lax.optimization_barrier(jnp.sum(weights, axis=1, keepdims=True))).astype(jnp.bfloat16)
        return jnp.dot(weights, value_head, preferred_element_type=jnp.float32).astype(jnp.bfloat16)
    heads_all = lax.map(one_head, jnp.arange(SEQUENCE_COUNT * HEADS, dtype=jnp.int32))
    heads_out = heads_all.reshape(SEQUENCE_COUNT, HEADS, SEQUENCE_LENGTH, HEAD_DIM).transpose(0, 2, 1, 3).reshape(SEQUENCE_COUNT * SEQUENCE_LENGTH, ATT)
    projected = jnp.dot(heads_out, out_weight, preferred_element_type=jnp.float32)
    residual_f = residual_in.reshape(SEQUENCE_COUNT * SEQUENCE_LENGTH, D).astype(jnp.float32)
    mixed_rows = residual_f + mix_gain * projected * lax.rsqrt(lax.optimization_barrier(jnp.mean(projected * projected, axis=1, keepdims=True)) + 1e-06)
    normed = (ffn_gain * mixed_rows * lax.rsqrt(lax.optimization_barrier(jnp.mean(mixed_rows * mixed_rows, axis=1, keepdims=True)) + 1e-06)).astype(jnp.bfloat16)
    gate_part = jnp.dot(normed, shared_gate, preferred_element_type=jnp.float32)
    up_part = jnp.dot(normed, shared_up, preferred_element_type=jnp.float32)
    shared_hidden = (jax.nn.silu(gate_part) * up_part).astype(jnp.bfloat16)
    shared_out = jnp.dot(shared_hidden, shared_down, preferred_element_type=jnp.float32)
    tokens_all = SEQUENCE_COUNT * SEQUENCE_LENGTH
    pair_total = tokens_all * TOPK
    sources = tokens_all // TOK_DEV
    per_source = TOK_DEV * TOPK
    id_blocks = expert_ids.reshape(sources, per_source)
    one_hot = (id_blocks[:, :, None] == jnp.arange(EXPERTS, dtype=jnp.int32)[None, None, :]).astype(jnp.int32)
    position_in = lax.optimization_barrier(jnp.sum((jnp.cumsum(one_hot, axis=1) - one_hot) * one_hot, axis=2))
    columns = jnp.arange(sources, dtype=jnp.int32)[:, None] * CAP + position_in
    pair_ids = jnp.arange(pair_total, dtype=jnp.int32).reshape(sources, per_source)
    table = jnp.full((EXPERTS, sources * CAP), pair_total, jnp.int32).at[id_blocks, columns].set(pair_ids)
    flat_weights = route_weights.reshape(pair_total)

    def one_expert(running, expert_index):
        pair_list = table[expert_index]
        is_valid = pair_list < pair_total
        token_list = jnp.where(is_valid, pair_list // TOPK, 0)
        weight_list = jnp.where(is_valid, flat_weights[jnp.minimum(pair_list, pair_total - 1)], 0.0)
        gathered = normed[token_list]
        gate_rows = jnp.dot(gathered, expert_gate[expert_index], preferred_element_type=jnp.float32)
        up_rows = jnp.dot(gathered, expert_up[expert_index], preferred_element_type=jnp.float32)
        hidden = (jax.nn.silu(gate_rows) * up_rows).astype(jnp.bfloat16)
        expert_out = jnp.dot(hidden, expert_down[expert_index], preferred_element_type=jnp.float32).astype(jnp.bfloat16)
        running = running.at[token_list].add(weight_list[:, None] * expert_out.astype(jnp.float32))
        return (running, None)
    routed, _ = lax.scan(one_expert, jnp.zeros((tokens_all, D), jnp.float32), jnp.arange(EXPERTS, dtype=jnp.int32))
    result_rows = (mixed_rows + shared_out + routed).astype(jnp.bfloat16)
    return result_rows.reshape(SEQUENCE_COUNT, SEQUENCE_LENGTH, D)
```

```python
import functools
import math

import jax
import jax.numpy as jnp
from jax import lax
from jax.experimental import pallas as pl
from jax.experimental.pallas import tpu as pltpu
from jax.sharding import PartitionSpec as P

HEAD_DIM = 64


def attend(query_all, key_all, value_all, gate_sums):
    length = query_all.shape[1]
    head_count = gate_sums.shape[1]
    score_scale = HEAD_DIM ** (-0.5)
    query_heads = query_all[0].reshape(length, head_count, HEAD_DIM)
    key_heads = key_all[0].reshape(length, head_count, HEAD_DIM)
    value_heads = value_all[0].reshape(length, head_count, HEAD_DIM)
    sums_local = gate_sums[0]
    block_rows = min(512, length)
    pieces = []
    for block_index in range(length // block_rows):
        start = block_index * block_rows
        block_end = start + block_rows
        scores = (
            jnp.einsum(
                "qhd,khd->hqk",
                query_heads[start:block_end],
                key_heads[:block_end],
                preferred_element_type=jnp.float32,
            )
            * score_scale
        )
        scores = scores + sums_local[:, start:block_end, None] - sums_local[:, None, :block_end]
        causal_mask = jnp.arange(block_end)[None, :] <= jnp.arange(start, block_end)[:, None]
        scores = jnp.where(causal_mask[None], scores, -jnp.inf)
        peak = jnp.max(scores, axis=2, keepdims=True)
        weights = jnp.exp(scores - peak)
        weights = (weights / jnp.sum(weights, axis=2, keepdims=True)).astype(jnp.bfloat16)
        mixed_heads = jnp.einsum(
            "hqk,khd->qhd", weights, value_heads[:block_end], preferred_element_type=jnp.float32
        ).astype(jnp.bfloat16)
        pieces.append(mixed_heads.reshape(block_rows, head_count * HEAD_DIM))
    return jnp.concatenate(pieces, axis=0)[None]


def gated_rows(rows_in, gate_w, up_w):
    gate_rows = jnp.dot(rows_in, gate_w, preferred_element_type=jnp.float32)
    up_rows = jnp.dot(rows_in, up_w, preferred_element_type=jnp.float32)
    return (jax.nn.silu(gate_rows) * up_rows).astype(jnp.bfloat16)


def shards(
    residual_in,
    query_rows,
    key_rows,
    value_rows,
    gate_sums,
    out_weight,
    mix_gain,
    ffn_gain,
    expert_ids,
    route_weights,
    expert_gate,
    expert_up,
    expert_down,
    shared_gate,
    shared_up,
    shared_down,
):
    query_all, key_all, value_all = (
        lax.all_to_all(query_rows, "sp", split_axis=2, concat_axis=1, tiled=True),
        lax.all_to_all(key_rows, "sp", split_axis=2, concat_axis=1, tiled=True),
        lax.all_to_all(value_rows, "sp", split_axis=2, concat_axis=1, tiled=True),
    )
    attended = attend(query_all, key_all, value_all, gate_sums)
    returned = lax.all_to_all(attended, "sp", split_axis=1, concat_axis=2, tiled=True)
    projected = jnp.dot(returned[0], out_weight, preferred_element_type=jnp.float32)
    residual_f = residual_in[0].astype(jnp.float32)
    mixed_rows = residual_f + mix_gain * projected * lax.rsqrt(
        jnp.mean(projected * projected, axis=1, keepdims=True) + 1e-06
    )
    normed = (
        ffn_gain
        * mixed_rows
        * lax.rsqrt(jnp.mean(mixed_rows * mixed_rows, axis=1, keepdims=True) + 1e-06)
    ).astype(jnp.bfloat16)
    shared_hidden = gated_rows(normed, shared_gate, shared_up)
    shared_out = jnp.dot(shared_hidden, shared_down, preferred_element_type=jnp.float32)
    tok_count = residual_in.shape[1]
    top_count = expert_ids.shape[2]
    width = residual_in.shape[2]
    sp_count = lax.axis_size("sp")
    dp_count = lax.axis_size("dp")
    expert_count = sp_count * dp_count
    capacity = 2 * tok_count * top_count // expert_count
    groups = math.gcd(sp_count, top_count)
    expert_list = expert_ids[0].reshape(tok_count * top_count)
    one_hot = (expert_list[:, None] == jnp.arange(expert_count, dtype=jnp.int32)[None, :]).astype(
        jnp.int32
    )
    position_in = jnp.sum((jnp.cumsum(one_hot, axis=0) - one_hot) * one_hot, axis=1)
    slot_index = (expert_list * capacity + position_in).reshape(tok_count, top_count)
    table = jnp.concatenate([slot_index.T.astype(jnp.float32), route_weights[0].T], axis=0)
    arrived, tables = dispatch(normed, table, groups, sp_count, dp_count, capacity)
    flat_rows = arrived.reshape(-1, width)
    hidden = gated_rows(flat_rows, expert_gate[0], expert_up[0])
    finished = jnp.dot(hidden, expert_down[0], preferred_element_type=jnp.float32).astype(
        jnp.bfloat16
    )
    result_rows = combine(
        finished.reshape(arrived.shape), tables, mixed_rows + shared_out, groups, sp_count, dp_count
    )
    return result_rows[None]


def places(groups, sp_count, dp_count):
    row_count = sp_count // groups
    sp_index = lax.axis_index("sp")
    dp_index = lax.axis_index("dp")
    layer = sp_index // row_count
    seat = (sp_index % row_count) * dp_count + dp_index

    def device_of(layer_to, seat_to):
        return {"sp": layer_to * row_count + seat_to // dp_count, "dp": seat_to % dp_count}

    return layer, seat, row_count * dp_count, device_of


def greet(layer, seat, groups, seats, device_of):
    barrier = pltpu.get_barrier_semaphore()
    for j in range(1, groups):
        pl.semaphore_signal(
            barrier, inc=1, device_id=device_of((layer + j) % groups, seat),
            device_id_type=pl.DeviceIdType.MESH,
        )

    @pl.loop(1, seats)
    def _(i):
        pl.semaphore_signal(
            barrier, inc=1, device_id=device_of(layer, (seat + i) % seats),
            device_id_type=pl.DeviceIdType.MESH,
        )

    pl.semaphore_wait(barrier, groups - 1 + seats - 1)


def remote(src, dst, send_sem, recv_sem, device):
    return pltpu.make_async_remote_copy(
        src_ref=src, dst_ref=dst, send_sem=send_sem, recv_sem=recv_sem,
        device_id=device, device_id_type=pl.DeviceIdType.MESH,
    )


def dispatch_kernel(
    groups, sp_count, dp_count, capacity, rows_ref, table_ref, out_ref, tables_out,
    all_rows, tables, picked, row_send, row_recv, table_send, table_recv, send, recv, own_sem,
):
    layer, seat, seats, device_of = places(groups, sp_count, dp_count)
    tok_count, width = rows_ref.shape
    top_count = table_ref.shape[0] // 2
    slots = seats * capacity
    step = min(512, width)
    greet(layer, seat, groups, seats, device_of)

    def row_copies(j):
        source = (layer - j + groups) % groups
        target = device_of((layer + j) % groups, seat)
        return (
            remote(table_ref, tables.at[layer], table_send.at[j], table_recv.at[j], target),
            remote(rows_ref, all_rows.at[layer], row_send.at[j], row_recv.at[j], target),
            remote(table_ref, tables.at[source], table_send.at[j], table_recv.at[j], target),
            remote(rows_ref, all_rows.at[source], row_send.at[j], row_recv.at[j], target),
        )

    for j in range(1, groups):
        for copy in row_copies(j)[:2]:
            copy.start()
    tables[layer] = table_ref[...]
    slot_rows = lax.broadcasted_iota(jnp.int32, (slots, tok_count), 0) + layer * slots
    slot_rows = slot_rows.astype(jnp.float32)

    for j in range(groups):
        source = (layer - j + groups) % groups
        if j > 0:
            for copy in row_copies(j)[2:]:
                copy.wait_recv()
        table = tables[source]
        choose = jnp.zeros((slots, tok_count), jnp.float32)
        for k in range(top_count):
            choose = choose + jnp.where(slot_rows == table[k : k + 1, :], 1.0, 0.0)
        choose = choose.astype(jnp.bfloat16)

        @pl.loop(0, width // step)
        def _(c):
            columns = pl.ds(pl.multiple_of(c * step, step), step)
            rows = rows_ref[:, columns] if j == 0 else all_rows[source, :, columns]
            value = jnp.dot(choose, rows, preferred_element_type=jnp.float32)
            for p in range(seats):
                picked[j, p, :, columns] = value[p * capacity : (p + 1) * capacity].astype(
                    jnp.bfloat16
                )

        @pl.loop(1, seats)
        def _(i):
            to = (seat + i) % seats
            remote(
                picked.at[j, to], out_ref.at[source, seat], send.at[j, i], recv.at[j, i],
                device_of(layer, to),
            ).start()

        pltpu.make_async_copy(picked.at[j, seat], out_ref.at[source, seat], own_sem.at[j]).start()

    tables_out[...] = tables[...]
    for j in range(groups):
        source = (layer - j + groups) % groups

        @pl.loop(1, seats)
        def _(i):
            to = (seat + i) % seats
            came = (seat - i + seats) % seats
            remote(
                picked.at[j, to], out_ref.at[source, came], send.at[j, i], recv.at[j, i],
                device_of(layer, to),
            ).wait()

        pltpu.make_async_copy(picked.at[j, seat], out_ref.at[source, seat], own_sem.at[j]).wait()
        if j > 0:
            for copy in row_copies(j)[:2]:
                copy.wait_send()


def dispatch(rows, table, groups, sp_count, dp_count, capacity):
    tok_count, width = rows.shape
    seats = sp_count * dp_count // groups
    vmem = pl.BlockSpec(memory_space=pltpu.VMEM)
    return pl.pallas_call(
        functools.partial(dispatch_kernel, groups, sp_count, dp_count, capacity),
        out_shape=(
            jax.ShapeDtypeStruct((groups, seats, capacity, width), jnp.bfloat16),
            jax.ShapeDtypeStruct((groups,) + table.shape, jnp.float32),
        ),
        in_specs=[vmem, vmem],
        out_specs=(pl.BlockSpec(memory_space=pl.ANY), vmem),
        scratch_shapes=[
            pltpu.VMEM((groups, tok_count, width), jnp.bfloat16),
            pltpu.VMEM((groups,) + table.shape, jnp.float32),
            pltpu.VMEM((groups, seats, capacity, width), jnp.bfloat16),
            pltpu.SemaphoreType.DMA((groups,)),
            pltpu.SemaphoreType.DMA((groups,)),
            pltpu.SemaphoreType.DMA((groups,)),
            pltpu.SemaphoreType.DMA((groups,)),
            pltpu.SemaphoreType.DMA((groups, seats)),
            pltpu.SemaphoreType.DMA((groups, seats)),
            pltpu.SemaphoreType.DMA((groups,)),
        ],
        compiler_params=pltpu.CompilerParams(collective_id=0, has_side_effects=True),
        name="dispatch",
    )(rows, table)


def combine_kernel(
    groups, sp_count, dp_count, done_ref, tables, base_ref, out_ref,
    back, partial, sums, send, recv, own_sem, sum_send, sum_recv,
):
    layer, seat, seats, device_of = places(groups, sp_count, dp_count)
    tok_count, width = base_ref.shape
    capacity = done_ref.shape[2]
    top_count = tables.shape[1] // 2
    slots = seats * capacity
    step = min(512, width)
    greet(layer, seat, groups, seats, device_of)
    order = list(range(1, groups)) + [0]

    def own_copy(j, source):
        return pltpu.make_async_copy(
            done_ref.at[source, seat], back.at[source, seat], own_sem.at[j]
        )

    for j in order:
        source = (layer - j + groups) % groups

        @pl.loop(1, seats)
        def _(i):
            to = (seat + i) % seats
            remote(
                done_ref.at[source, to], back.at[source, seat], send.at[j, i], recv.at[j, i],
                device_of(layer, to),
            ).start()

        own_copy(j, source).start()

    slot_rows = lax.broadcasted_iota(jnp.int32, (slots, tok_count), 0) + layer * slots
    slot_rows = slot_rows.astype(jnp.float32)

    for j in order:
        source = (layer - j + groups) % groups

        @pl.loop(1, seats)
        def _(i):
            to = (seat + i) % seats
            came = (seat - i + seats) % seats
            remote(
                done_ref.at[source, to], back.at[source, came], send.at[j, i], recv.at[j, i],
                device_of(layer, to),
            ).wait()

        own_copy(j, source).wait()
        if j == 0:
            for other in range(1, groups):
                remote(
                    partial.at[other], sums.at[other], sum_send.at[other], sum_recv.at[other],
                    device_of((layer - other + groups) % groups, seat),
                ).wait()
        table = tables[source]
        weigh = jnp.zeros((slots, tok_count), jnp.float32)
        for k in range(top_count):
            weigh = weigh + jnp.where(
                slot_rows == table[k : k + 1, :], table[top_count + k : top_count + k + 1, :], 0.0
            )
        weigh = weigh.T
        high = weigh.astype(jnp.bfloat16)
        low = (weigh - high.astype(jnp.float32)).astype(jnp.bfloat16)

        @pl.loop(0, width // step)
        def _(c):
            columns = pl.ds(pl.multiple_of(c * step, step), step)
            rows = back[source, :, :, columns]
            if capacity % 16:
                rows = rows.astype(jnp.float32).reshape(slots, step).astype(jnp.bfloat16)
            else:
                rows = rows.reshape(slots, step)
            value = jnp.dot(high, rows, preferred_element_type=jnp.float32) + jnp.dot(
                low, rows, preferred_element_type=jnp.float32
            )
            if j == 0:
                total = base_ref[:, columns] + value
                for other in range(1, groups):
                    total = total + sums[other, :, columns].astype(jnp.float32)
                out_ref[:, columns] = total.astype(jnp.bfloat16)
            else:
                partial[j, :, columns] = value.astype(jnp.bfloat16)

        if j > 0:
            remote(
                partial.at[j], sums.at[j], sum_send.at[j], sum_recv.at[j], device_of(source, seat)
            ).start()


def combine(finished, tables, base, groups, sp_count, dp_count):
    tok_count, width = base.shape
    seats = finished.shape[1]
    vmem = pl.BlockSpec(memory_space=pltpu.VMEM)
    return pl.pallas_call(
        functools.partial(combine_kernel, groups, sp_count, dp_count),
        out_shape=jax.ShapeDtypeStruct(base.shape, jnp.bfloat16),
        in_specs=[pl.BlockSpec(memory_space=pl.ANY), vmem, vmem],
        out_specs=vmem,
        scratch_shapes=[
            pltpu.VMEM(finished.shape, jnp.bfloat16),
            pltpu.VMEM((groups, tok_count, width), jnp.bfloat16),
            pltpu.VMEM((groups, tok_count, width), jnp.bfloat16),
            pltpu.SemaphoreType.DMA((groups, seats)),
            pltpu.SemaphoreType.DMA((groups, seats)),
            pltpu.SemaphoreType.DMA((groups,)),
            pltpu.SemaphoreType.DMA((groups,)),
            pltpu.SemaphoreType.DMA((groups,)),
        ],
        compiler_params=pltpu.CompilerParams(collective_id=1, has_side_effects=True),
        name="combine",
    )(finished, tables, base)


def solution(mesh):
    return jax.shard_map(
        shards,
        mesh=mesh,
        in_specs=(
            P("dp", "sp", None),
            P("dp", "sp", None),
            P("dp", "sp", None),
            P("dp", "sp", None),
            P("dp", "sp", None),
            P(),
            P(),
            P(),
            P("dp", "sp", None),
            P("dp", "sp", None),
            P(("sp", "dp"), None, None),
            P(("sp", "dp"), None, None),
            P(("sp", "dp"), None, None),
            P(),
            P(),
            P(),
        ),
        out_specs=P("dp", "sp", None),
        check_vma=False,
    )
```
